32 devices in a mesh: grp: 2 (over y), ep: 4 (over z), tp: 4 (over x, core).
Axes of the slice: x: 2, y: 2, z: 4, core: 2. Of those that a mesh axis runs over, the one named last changes fastest.
Arguments:
- tokens: bfloat16 [2048, 2048], P(('grp', 'ep')), parts along dimension 0, may hold values from -6 to 6
- norm_gain: float32 [2048], replicated, may hold values from 0.1 to 1.9
- routing: int32 [2048, 2], P(('grp', 'ep')), parts along dimension 0, may hold values from 0 to 3, all different within a row; in each aligned block of 256 rows (0 to 255, 256 to 511, ...) at most 192 rows name the same one
- gate_weights: float32 [2048, 2], P(('grp', 'ep')), parts along dimension 0, may hold values from 0.2 to 2
- expert_gate: bfloat16 [4, 2048, 1024], P('ep', None, 'tp'), may hold values from -0.125 to 0.125
- expert_up: bfloat16 [4, 2048, 1024], P('ep', None, 'tp'), may hold values from -0.125 to 0.125
- expert_down: bfloat16 [4, 1024, 2048], P('ep', 'tp'), may hold values from -0.1875 to 0.1875
- shared_gate: bfloat16 [2048, 512], P(None, 'tp'), may hold values from -0.125 to 0.125
- shared_up: bfloat16 [2048, 512], P(None, 'tp'), may hold values from -0.125 to 0.125
- shared_down: bfloat16 [512, 2048], P('tp'), may hold values from -0.25 to 0.25
Outputs:
- mixed: bfloat16 [2048, 2048], P(('grp', 'ep'), 'tp'), parts along dimension 0
The draws below stay inside these ranges and needn't reach their ends.
There are 2 independent parts, one for each index of `grp`. The reference program is written for one: setup_inputs(seed, part) draws one part's arguments, and reference() takes and returns one part's arrays. A program takes and returns all parts, laid end to end along the dimension named above; an argument that names none is the same for every part. Nothing has to cross between parts.
Inputs may be any that keep to these rules, and one draw needn't show every extreme that they name: `routing`: each row names 2 different experts. Within each aligned block of 256 rows no expert is named by more than 192 rows, and in every draw some block has an expert named by exactly 192 rows.
All inputs are finite; a program needn't handle non-finite values.
Results may differ from the reference program's by a relative error of at most 0.012.
Values may be sent and summed in bfloat16 or wider, within the bound.
A program may use at most 64 MiB of HBM per device.

```python
import math
import jax
import jax.numpy as jnp
import numpy as np
from jax import lax

D = 2048
FFE = 1024
FFS = 512
TOP_K = 2
TOK_DEV = 256
EXPERTS = 4
CAP = 192
TOKENS = 1024
N_EP = 4
N_TP = 4


def level_of(rng, extent, pieces, smallest, top_value):
    def one(axis_at, shards_of):
        heights = jax.random.uniform(jax.random.fold_in(jax.random.fold_in(rng, 6), axis_at), (shards_of,), jnp.float32, smallest / len(pieces), top_value / len(pieces))
        return jnp.repeat(jnp.exp(heights), extent[axis_at] // shards_of).reshape((-1,) + (1,) * (len(extent) - axis_at - 1))

    factor_of = one(*pieces[0])
    for cut in pieces[1:]:
        factor_of = factor_of * one(*cut)
    return factor_of


def routed_block(stream_key, own, number, rows, count, top, most, slope):
    ranking = jax.random.permutation(stream_key, count)
    heavy_load, ordinary = shares(count, rows * top, most, slope, True), shares(count, rows * top, most, slope, False)
    places = jnp.arange(count)

    def named(tallies, rotation):
        used = int((tallies > 0).sum())
        fixed = max(1, used // 4)
        shifted = fixed + (places - fixed + rotation * (used - fixed)) % max(1, count - fixed)
        return jnp.zeros((count,), jnp.int32).at[ranking[jnp.where(places < fixed, places, shifted)]].set(jnp.asarray(tallies, jnp.int32))

    tallies = jnp.where(number % 4 == 0, named(heavy_load, number // 4), named(ordinary, number - number // 4 - 1))
    mixed = jax.random.permutation(jax.random.fold_in(own, 3), count)
    giver, taker = mixed[0:count // 2 * 2:2], mixed[1:count // 2 * 2:2]
    room = jnp.minimum(tallies[giver] - 1, most - tallies[taker]) // 2
    room = jnp.where((giver == ranking[0]) | (taker == ranking[0]) | (tallies[taker] == 0), 0, jnp.maximum(room, 0))
    shifted = jax.random.randint(jax.random.fold_in(own, 4), (count // 2,), 0, 1 << 20) % (room + 1)
    tallies = tallies.at[giver].add(-shifted).at[taker].add(shifted)
    items = jnp.searchsorted(jnp.cumsum(tallies), jnp.arange(rows * top), side="right").astype(jnp.int32)
    grid = items.reshape(top, rows).T
    grid = grid[jax.random.permutation(jax.random.fold_in(own, 1), rows)]
    rotation = jax.random.randint(jax.random.fold_in(own, 2), (rows, 1), 0, top)
    return jnp.take_along_axis(grid, (jnp.arange(top)[None, :] + rotation) % top, axis=1)


def shares(number_of, total, limit, skew, full):
    portions = [(1 << 20) // math.isqrt(grade ** skew) + 1 for grade in range(1, number_of + 1)]
    largest = limit if full else min(limit, max(-(-total // number_of), total * portions[0] // sum(portions)))
    least = 1 if total - largest >= number_of - 1 else 0
    holding, rest = [largest] + [least] * (number_of - 1), total - largest - least * (number_of - 1)
    while rest > 0:
        free = [i for i in range(1, number_of) if holding[i] < largest] or [i for i in range(1, number_of) if holding[i] < limit]
        mass, remaining = sum([portions[i] for i in free]), rest
        for i in free:
            addition = min(limit - holding[i], max(1, remaining * portions[i] // mass), rest)
            holding[i] = holding[i] + addition
            rest = rest - addition
    return np.array(holding)


def bell_draw(own_key, dims, scale, reach, cuts=(), held_as=jnp.bfloat16):
    gain = level_of(own_key, dims, cuts, -0.22, 0.18) if cuts else 1.0
    result = jax.random.normal(own_key, dims, jnp.float32) * scale * gain
    return jnp.minimum(jnp.maximum(result, -reach), reach).astype(held_as)


def setup_inputs(seed: int = 0, part: int = 0) -> dict:
    streams_of = jax.random.split(jax.random.key(seed), 11)
    part_keys = jax.random.split(jax.random.fold_in(streams_of[10], part), 11)
    tokens = bell_draw(part_keys[0], (TOKENS, D), 1.0, 6.0, ((0, 4),))
    norm_gain = jnp.clip(1.0 + 0.18 * jax.random.normal(streams_of[1], (D,), jnp.float32), 0.1, 1.9)
    routing_keys = jax.random.split(jax.random.fold_in(part_keys[2], 1), TOKENS // TOK_DEV)
    routing_turns = jax.random.permutation(jax.random.fold_in(part_keys[2], 3), TOKENS // TOK_DEV)
    routing = jax.vmap(lambda own, number: routed_block(jax.random.fold_in(part_keys[2], 2), own, number, TOK_DEV, EXPERTS, TOP_K, CAP, 2))(routing_keys, routing_turns).reshape((TOKENS, TOP_K))
    gate_weights = jnp.clip(jnp.exp(math.log(2.0) - 2.3025851 * jax.random.uniform(part_keys[3], (TOKENS, TOP_K), jnp.float32) ** level_of(part_keys[3], (TOKENS, TOP_K), ((0, 4),), -0.2, 0.2)), 0.2, 2.0)
    expert_gate = bell_draw(streams_of[4], (EXPERTS, D, FFE), D ** -0.5, 0.125, ((0, 4), (2, 4)))
    expert_up = bell_draw(streams_of[5], (EXPERTS, D, FFE), D ** -0.5, 0.125, ((0, 4), (2, 4)))
    expert_down = bell_draw(streams_of[6], (EXPERTS, FFE, D), FFE ** -0.5, 0.1875, ((0, 4), (1, 4)))
    shared_gate = bell_draw(streams_of[7], (D, FFS), D ** -0.5, 0.125, ((1, 4),))
    shared_up = bell_draw(streams_of[8], (D, FFS), D ** -0.5, 0.125, ((1, 4),))
    shared_down = bell_draw(streams_of[9], (FFS, D), FFS ** -0.5, 0.25, ((0, 4),))
    return dict(tokens=tokens, norm_gain=norm_gain, routing=routing, gate_weights=gate_weights, expert_gate=expert_gate, expert_up=expert_up, expert_down=expert_down, shared_gate=shared_gate, shared_up=shared_up, shared_down=shared_down)


def norm_rows(tokens, norm_gain):
    values = tokens.astype(jnp.float32)
    scale = lax.rsqrt(lax.optimization_barrier(jnp.mean(values * values, axis=-1, keepdims=True)) + 1e-06)
    return (values * scale * norm_gain).astype(jnp.bfloat16)

def grouped_down(hidden, down):
    width = hidden.shape[1] // N_TP
    total = jnp.zeros((hidden.shape[0], down.shape[1]), jnp.float32)
    for group in range(N_TP):
        partial_sum = jnp.dot(hidden[:, group * width:(group + 1) * width], down[group * width:(group + 1) * width], preferred_element_type=jnp.float32)
        total = total + partial_sum.astype(jnp.bfloat16).astype(jnp.float32)
    return total

def swiglu_hidden(rows, w_gate, w_up):
    gate = jnp.dot(rows, w_gate, preferred_element_type=jnp.float32)
    up = jnp.dot(rows, w_up, preferred_element_type=jnp.float32)
    return (jax.nn.silu(gate) * up).astype(jnp.bfloat16)

def reference(tokens, norm_gain, routing, gate_weights, expert_gate, expert_up, expert_down, shared_gate, shared_up, shared_down):
    normed = norm_rows(tokens, norm_gain)
    assign = TOK_DEV * TOP_K
    blocks = routing.reshape(N_EP, assign).astype(jnp.int32)
    onehot = (blocks[:, :, None] == jnp.arange(EXPERTS, dtype=jnp.int32)[None, None, :]).astype(jnp.int32)
    slot = lax.optimization_barrier(jnp.sum(jnp.cumsum(onehot, axis=1) * onehot, axis=2)).astype(jnp.int32) - 1
    dest = blocks * CAP + slot
    owner = (jnp.arange(N_EP, dtype=jnp.int32)[:, None] * TOK_DEV + jnp.arange(assign, dtype=jnp.int32)[None, :] // TOP_K).astype(jnp.int32)

    def fill_table(where, who):
        return jnp.full((EXPERTS * CAP,), TOKENS, jnp.int32).at[where].set(who)
    table = jax.vmap(fill_table)(dest, owner)
    table = table.reshape(N_EP, EXPERTS, CAP).transpose(1, 0, 2).reshape(EXPERTS, N_EP * CAP)
    padded = jnp.concatenate([normed, jnp.zeros((1, D), jnp.bfloat16)], axis=0)

    def one_expert(items):
        index, w_gate, w_up, w_down = items
        hidden = swiglu_hidden(padded[index], w_gate, w_up)
        return grouped_down(hidden, w_down).astype(jnp.bfloat16)
    outputs = lax.map(one_expert, (table, expert_gate, expert_up, expert_down))
    flat_index = blocks * (N_EP * CAP) + jnp.arange(N_EP, dtype=jnp.int32)[:, None] * CAP + slot
    picked = outputs.reshape(EXPERTS * N_EP * CAP, D)[flat_index.reshape(TOKENS * TOP_K)]
    picked = picked.astype(jnp.float32).reshape(TOKENS, TOP_K, D)
    routed = lax.optimization_barrier(jnp.sum(picked * gate_weights[:, :, None], axis=1))
    shared_out = grouped_down(swiglu_hidden(normed, shared_gate, shared_up), shared_down)
    return (routed + shared_out).astype(jnp.bfloat16)
```

```python
import jax
import jax.numpy as jnp
from jax import lax
from jax.experimental import pallas as pl
from jax.experimental.pallas import tpu as pltpu
from jax.sharding import PartitionSpec as P


def norm_rows(tokens, norm_gain):
    values = tokens.astype(jnp.float32)
    scale = lax.rsqrt(jnp.mean(values * values, axis=-1, keepdims=True) + 1e-06)
    return (values * scale * norm_gain).astype(jnp.bfloat16)


def body(
    tokens,
    norm_gain,
    routing,
    gate_weights,
    expert_gate,
    expert_up,
    expert_down,
    shared_gate,
    shared_up,
    shared_down,
):
    ep_count = lax.axis_size("ep")
    tp_count = lax.axis_size("tp")
    tok_rows, width = tokens.shape
    top = routing.shape[1]
    local_experts = expert_gate.shape[0]
    experts = ep_count * local_experts
    capacity = max(2, 3 * tok_rows * top // (2 * experts))
    quarter = width // tp_count
    arrived_rows = ep_count * capacity
    normed = norm_rows(tokens, norm_gain)
    flat_experts = routing.reshape(-1)
    assign = flat_experts.shape[0]
    onehot = (flat_experts[:, None] == jnp.arange(experts, dtype=jnp.int32)[None, :]).astype(
        jnp.float32
    )
    lower = (jnp.arange(assign)[:, None] >= jnp.arange(assign)[None, :]).astype(jnp.float32)
    running = jnp.dot(lower, onehot, precision=lax.Precision.HIGHEST)
    slot = (jnp.sum(running * onehot, axis=1) - 1.0).astype(jnp.int32)
    dest = flat_experts * capacity + slot
    owner = jnp.arange(assign, dtype=jnp.int32) // top
    slot_token = jnp.full((experts * capacity,), tok_rows, jnp.int32).at[dest].set(owner)
    padded = jnp.concatenate([normed, jnp.zeros((1, width), jnp.bfloat16)], axis=0)
    outgoing = padded[slot_token].reshape(experts, capacity, width)
    position = lax.axis_index("tp")
    own_columns = lax.dynamic_slice_in_dim(outgoing, position * quarter, quarter, 2)
    arrived = lax.all_to_all(own_columns, "ep", split_axis=0, concat_axis=0, tiled=True)
    piece = lax.all_gather(arrived, "tp", axis=2, tiled=True)
    count = piece.shape[2]
    piece = piece.reshape(ep_count, local_experts, capacity, count)
    local = 0
    rows = piece[:, local].reshape(arrived_rows, count)
    gate_rows = expert_gate[local]
    up_rows = expert_up[local]
    gate_list = [jnp.dot(rows, gate_rows, preferred_element_type=jnp.float32)]
    up_list = [jnp.dot(rows, up_rows, preferred_element_type=jnp.float32)]
    gate_all = jnp.stack(gate_list)
    up_all = jnp.stack(up_list)
    local = 0
    hidden = (jax.nn.silu(gate_all[local]) * up_all[local]).astype(jnp.bfloat16)
    term = jnp.dot(hidden, expert_down[local], preferred_element_type=jnp.float32)
    routed_list = [term.reshape(ep_count, capacity, width)]
    routed_terms = jnp.stack(routed_list, axis=1).reshape(experts * capacity, width)
    shared_gate_rows = jnp.dot(normed, shared_gate, preferred_element_type=jnp.float32)
    shared_up_rows = jnp.dot(normed, shared_up, preferred_element_type=jnp.float32)
    shared_hidden = (jax.nn.silu(shared_gate_rows) * shared_up_rows).astype(jnp.bfloat16)
    shared_term = jnp.dot(shared_hidden, shared_down, preferred_element_type=jnp.float32)
    routed_sum, shared_sum = (
        lax.psum_scatter(
            routed_terms.astype(jnp.bfloat16), "tp", scatter_dimension=1, tiled=True
        ).astype(jnp.float32),
        lax.psum_scatter(
            shared_term.astype(jnp.bfloat16), "tp", scatter_dimension=1, tiled=True
        ).astype(jnp.float32),
    )
    expert_out = routed_sum.astype(jnp.bfloat16).reshape(experts, capacity, quarter)
    returned = lax.all_to_all(expert_out, "ep", split_axis=0, concat_axis=0, tiled=True)
    picked = returned.reshape(experts * capacity, quarter)[dest]
    picked = picked.astype(jnp.float32).reshape(tok_rows, top, quarter)
    routed = jnp.sum(picked * gate_weights[:, :, None], axis=1)
    return (routed + shared_sum).astype(jnp.bfloat16)


MESH = pl.DeviceIdType.MESH


def silu(v):
    return v / (1.0 + jnp.exp(-v))


def dot32(a, b):
    return jnp.dot(a, b, preferred_element_type=jnp.float32)


def make_kernel(ep_count, capacity):
    others = list(range(1, ep_count))

    def kernel(
        tok_ref, gain_ref, routing_ref, gw_ref, wg_hbm, wu_hbm, wd_hbm, sg_hbm, su_hbm, sd_hbm,
        out_ref,
        wg, wu, wd, sg, su, sd, nq, pt, zsend, xq, esend, erecv, keep, fsend, frecv, gsend, grecv,
        wsem, zs, zr, cs, cr, xs, xr, ds, dr, es, er, fs, fr, gs, gr,
    ):
        e = lax.axis_index("ep")
        t = lax.axis_index("tp")
        x = t // 2
        c = t % 2
        core = {"tp": t ^ 1}
        across = {"tp": t ^ 2}
        rows, width = tok_ref.shape
        quarter = width // 4

        barrier = pltpu.get_barrier_semaphore()
        for k in others:
            pl.semaphore_signal(barrier, inc=1, device_id={"ep": e ^ k}, device_id_type=MESH)
        pl.semaphore_signal(barrier, inc=1, device_id=core, device_id_type=MESH)
        pl.semaphore_signal(barrier, inc=1, device_id=across, device_id_type=MESH)

        loads = [
            pltpu.make_async_copy(a, b, wsem.at[i])
            for i, (a, b) in enumerate(
                [(wg_hbm, wg), (wu_hbm, wu), (sg_hbm, sg), (su_hbm, su), (wd_hbm, wd), (sd_hbm, sd)]
            )
        ]
        for load in loads:
            load.start()

        values = tok_ref[...].astype(jnp.float32)
        scale = lax.rsqrt(jnp.mean(values * values, axis=-1, keepdims=True) + 1e-06)
        normed = (values * scale * gain_ref[...]).astype(jnp.bfloat16)
        for q in range(4):
            nq[q] = normed[:, q * quarter:(q + 1) * quarter]

        lane = lax.broadcasted_iota(jnp.int32, (rows, 128), 1)
        named = lane ^ e
        hit = jnp.where(routing_ref[:, 0:1] == named, 1.0, 0.0)
        weight = jnp.where(routing_ref[:, 0:1] == named, gw_ref[:, 0:1], 0.0)
        for j in range(1, routing_ref.shape[1]):
            hit = hit + jnp.where(routing_ref[:, j:j + 1] == named, 1.0, 0.0)
            weight = weight + jnp.where(routing_ref[:, j:j + 1] == named, gw_ref[:, j:j + 1], 0.0)
        earlier = (
            lax.broadcasted_iota(jnp.int32, (rows, rows), 0)
            > lax.broadcasted_iota(jnp.int32, (rows, rows), 1)
        )
        earlier = jnp.where(earlier, 1.0, 0.0).astype(jnp.bfloat16)
        rank = dot32(earlier, hit.astype(jnp.bfloat16))
        rank = jnp.where(hit > 0.5, rank, -1.0)
        place = lax.broadcasted_iota(jnp.int32, (rows, capacity), 1).astype(jnp.float32)

        def remote(src, dst, send, recv, to):
            return pltpu.make_async_remote_copy(
                src_ref=src, dst_ref=dst, send_sem=send, recv_sem=recv,
                device_id=to, device_id_type=MESH,
            )

        zcopy, ccopy, xcopy, dcopy, ecopy, fcopy, gcopy = {}, {}, {}, {}, {}, {}, {}
        for k in others:
            i = k - 1
            chosen = jnp.where(rank[:, k:k + 1] == place, 1.0, 0.0).astype(jnp.bfloat16)
            pt[i] = chosen
            packed = lax.dot_general(
                chosen, nq[t], (((0,), (0,)), ((), ())), preferred_element_type=jnp.float32
            )
            zsend[i] = packed.astype(jnp.bfloat16)
            if k == others[0]:
                pl.semaphore_wait(barrier, len(others) + 2)
            zcopy[k] = remote(zsend.at[i], xq.at[i, t], zs.at[i], zr.at[i], {"ep": e ^ k})
            zcopy[k].start()

        def columns(q):
            return pl.ds(pl.multiple_of(q * quarter, quarter), quarter)

        def hidden_of(pieces, w_gate, w_up):
            gate, up = 0.0, 0.0
            for q in range(4):
                gate = gate + dot32(pieces(q), w_gate[q * quarter:(q + 1) * quarter, :])
                up = up + dot32(pieces(q), w_up[q * quarter:(q + 1) * quarter, :])
            return (silu(gate) * up).astype(jnp.bfloat16)

        def exchange(r, n, product):
            for j in range(2):
                esend[r, j, :n] = product(columns(2 * j + 1 - c)).astype(jnp.bfloat16)
            ecopy[r] = remote(
                esend.at[r, :, pl.ds(0, n)], erecv.at[r, :, pl.ds(0, n)], es.at[r], er.at[r], core
            )
            ecopy[r].start()
            for j in range(2):
                keep[r, j, :n] = product(columns(2 * j + c))

        def arrive(k):
            i = k - 1
            zcopy[k].wait_recv()
            mine = xq.at[i, t]
            xcopy[k] = remote(mine, mine, xs.at[i], xr.at[i], across)
            xcopy[k].start()
            ccopy[k] = remote(mine, mine, cs.at[i], cr.at[i], core)
            ccopy[k].start()

        def relay(k):
            i = k - 1
            xcopy[k].wait_recv()
            theirs = xq.at[i, t ^ 2]
            dcopy[k] = remote(theirs, theirs, ds.at[i], dr.at[i], core)
            dcopy[k].start()

        def expert(k):
            i = k - 1
            ccopy[k].wait_recv()
            dcopy[k].wait_recv()
            hidden = hidden_of(lambda q: xq[i, q], wg, wu)
            exchange(k, capacity, lambda cols: dot32(hidden, wd[:, cols]))

        def pair(r, n):
            ecopy[r].wait_recv()
            fsend[r, :n] = (
                keep[r, 1 - x, :n] + erecv[r, 1 - x, :n].astype(jnp.float32)
            ).astype(jnp.bfloat16)
            fcopy[r] = remote(
                fsend.at[r, pl.ds(0, n)], frecv.at[r, pl.ds(0, n)], fs.at[r], fr.at[r], across
            )
            fcopy[r].start()

        def whole(r, n):
            fcopy[r].wait_recv()
            return (
                keep[r, x, :n]
                + erecv[r, x, :n].astype(jnp.float32)
                + frecv[r, :n].astype(jnp.float32)
            )

        def give_back(k):
            i = k - 1
            gsend[i] = whole(k, capacity).astype(jnp.bfloat16)
            gcopy[k] = remote(gsend.at[i], grecv.at[i], gs.at[i], gr.at[i], {"ep": e ^ k})
            gcopy[k].start()

        for load in loads:
            load.wait()
        own_hidden = hidden_of(lambda q: nq[q], wg, wu)
        shared_hidden = hidden_of(lambda q: nq[q], sg, su)
        exchange(
            0,
            rows,
            lambda cols: dot32(own_hidden, wd[:, cols]) * weight[:, 0:1]
            + dot32(shared_hidden, sd[:, cols]),
        )
        plan(arrive, relay, expert, pair, give_back, others, rows, capacity)

        total = whole(0, rows)
        for k in others:
            gcopy[k].wait_recv()
            total = total + dot32(pt[k - 1], grecv[k - 1]) * weight[:, k:k + 1]
        out_ref[...] = total.astype(out_ref.dtype)

        for group in (zcopy, ccopy, xcopy, dcopy, ecopy, fcopy, gcopy):
            for copy in group.values():
                copy.wait_send()

    return kernel


def plan(arrive, relay, expert, pair, give_back, others, rows, capacity):
    previous = None
    for k in others:
        arrive(k)
        if previous is None:
            pair(0, rows)
        else:
            give_back(previous)
        relay(k)
        expert(k)
        pair(k, capacity)
        previous = k
    give_back(previous)


def fused_body(
    tokens, norm_gain, routing, gate_weights,
    expert_gate, expert_up, expert_down, shared_gate, shared_up, shared_down,
):
    n = lax.axis_size("ep")
    rows, width = tokens.shape
    capacity = max(2, 3 * rows * routing.shape[1] // (2 * n))
    quarter = width // 4
    ffe = expert_gate.shape[2]
    ffs = shared_gate.shape[1]
    o = n - 1
    bf16, f32 = jnp.bfloat16, jnp.float32
    big = max(rows, capacity)
    dma = pltpu.SemaphoreType.DMA
    vmem = pl.BlockSpec(memory_space=pltpu.VMEM)
    hbm = pl.BlockSpec(memory_space=pl.ANY)
    return pl.pallas_call(
        make_kernel(n, capacity),
        out_shape=jax.ShapeDtypeStruct((rows, quarter), bf16),
        in_specs=[vmem] * 4 + [hbm] * 6,
        out_specs=vmem,
        scratch_shapes=[
            pltpu.VMEM((width, ffe), bf16),
            pltpu.VMEM((width, ffe), bf16),
            pltpu.VMEM((ffe, width), bf16),
            pltpu.VMEM((width, ffs), bf16),
            pltpu.VMEM((width, ffs), bf16),
            pltpu.VMEM((ffs, width), bf16),
            pltpu.VMEM((4, rows, quarter), bf16),
            pltpu.VMEM((o, rows, capacity), bf16),
            pltpu.VMEM((o, capacity, quarter), bf16),
            pltpu.VMEM((o, 4, capacity, quarter), bf16),
            pltpu.VMEM((n, 2, big, quarter), bf16),
            pltpu.VMEM((n, 2, big, quarter), bf16),
            pltpu.VMEM((n, 2, big, quarter), f32),
            pltpu.VMEM((n, big, quarter), bf16),
            pltpu.VMEM((n, big, quarter), bf16),
            pltpu.VMEM((o, capacity, quarter), bf16),
            pltpu.VMEM((o, capacity, quarter), bf16),
            dma((6,)),
        ]
        + [dma((o,))] * 8
        + [dma((n,))] * 4
        + [dma((o,))] * 2,
        compiler_params=pltpu.CompilerParams(collective_id=0, has_side_effects=True),
    )(
        tokens, norm_gain.reshape(1, width), routing, gate_weights,
        expert_gate[0], expert_up[0], expert_down[0], shared_gate, shared_up, shared_down,
    )


def solution(mesh):
    in_specs = (
        P(("grp", "ep"), None),
        P(),
        P(("grp", "ep"), None),
        P(("grp", "ep"), None),
        P("ep", None, "tp"),
        P("ep", None, "tp"),
        P("ep", "tp", None),
        P(None, "tp"),
        P(None, "tp"),
        P("tp", None),
    )
    out_specs = P(("grp", "ep"), "tp")
    ep_count, tp_count = mesh.shape["ep"], mesh.shape["tp"]

    def layer(*args):
        few = tp_count == 4 and ep_count in (2, 4) and args[4].shape[0] == ep_count
        chosen = fused_body if few else body
        return jax.shard_map(
            chosen, mesh=mesh, in_specs=in_specs, out_specs=out_specs, check_vma=False
        )(*args)

    return layer
```

```python
import jax
import jax.numpy as jnp
from jax import lax
from jax.experimental import pallas as pl
from jax.experimental.pallas import tpu as pltpu
from jax.sharding import PartitionSpec as P


def norm_rows(tokens, norm_gain):
    values = tokens.astype(jnp.float32)
    scale = lax.rsqrt(jnp.mean(values * values, axis=-1, keepdims=True) + 1e-06)
    return (values * scale * norm_gain).astype(jnp.bfloat16)


def body(
    tokens,
    norm_gain,
    routing,
    gate_weights,
    expert_gate,
    expert_up,
    expert_down,
    shared_gate,
    shared_up,
    shared_down,
):
    ep_count = lax.axis_size("ep")
    tp_count = lax.axis_size("tp")
    tok_rows, width = tokens.shape
    top = routing.shape[1]
    local_experts = expert_gate.shape[0]
    experts = ep_count * local_experts
    capacity = max(2, 3 * tok_rows * top // (2 * experts))
    quarter = width // tp_count
    arrived_rows = ep_count * capacity
    normed = norm_rows(tokens, norm_gain)
    flat_experts = routing.reshape(-1)
    assign = flat_experts.shape[0]
    onehot = (flat_experts[:, None] == jnp.arange(experts, dtype=jnp.int32)[None, :]).astype(
        jnp.float32
    )
    lower = (jnp.arange(assign)[:, None] >= jnp.arange(assign)[None, :]).astype(jnp.float32)
    running = jnp.dot(lower, onehot, precision=lax.Precision.HIGHEST)
    slot = (jnp.sum(running * onehot, axis=1) - 1.0).astype(jnp.int32)
    dest = flat_experts * capacity + slot
    owner = jnp.arange(assign, dtype=jnp.int32) // top
    slot_token = jnp.full((experts * capacity,), tok_rows, jnp.int32).at[dest].set(owner)
    padded = jnp.concatenate([normed, jnp.zeros((1, width), jnp.bfloat16)], axis=0)
    outgoing = padded[slot_token].reshape(experts, capacity, width)
    position = lax.axis_index("tp")
    own_columns = lax.dynamic_slice_in_dim(outgoing, position * quarter, quarter, 2)
    arrived = lax.all_to_all(own_columns, "ep", split_axis=0, concat_axis=0, tiled=True)
    piece = lax.all_gather(arrived, "tp", axis=2, tiled=True)
    count = piece.shape[2]
    piece = piece.reshape(ep_count, local_experts, capacity, count)
    local = 0
    rows = piece[:, local].reshape(arrived_rows, count)
    gate_rows = expert_gate[local]
    up_rows = expert_up[local]
    gate_list = [jnp.dot(rows, gate_rows, preferred_element_type=jnp.float32)]
    up_list = [jnp.dot(rows, up_rows, preferred_element_type=jnp.float32)]
    gate_all = jnp.stack(gate_list)
    up_all = jnp.stack(up_list)
    local = 0
    hidden = (jax.nn.silu(gate_all[local]) * up_all[local]).astype(jnp.bfloat16)
    term = jnp.dot(hidden, expert_down[local], preferred_element_type=jnp.float32)
    routed_list = [term.reshape(ep_count, capacity, width)]
    routed_terms = jnp.stack(routed_list, axis=1).reshape(experts * capacity, width)
    shared_gate_rows = jnp.dot(normed, shared_gate, preferred_element_type=jnp.float32)
    shared_up_rows = jnp.dot(normed, shared_up, preferred_element_type=jnp.float32)
    shared_hidden = (jax.nn.silu(shared_gate_rows) * shared_up_rows).astype(jnp.bfloat16)
    shared_term = jnp.dot(shared_hidden, shared_down, preferred_element_type=jnp.float32)
    routed_sum, shared_sum = (
        lax.psum_scatter(
            routed_terms.astype(jnp.bfloat16), "tp", scatter_dimension=1, tiled=True
        ).astype(jnp.float32),
        lax.psum_scatter(
            shared_term.astype(jnp.bfloat16), "tp", scatter_dimension=1, tiled=True
        ).astype(jnp.float32),
    )
    expert_out = routed_sum.astype(jnp.bfloat16).reshape(experts, capacity, quarter)
    returned = lax.all_to_all(expert_out, "ep", split_axis=0, concat_axis=0, tiled=True)
    picked = returned.reshape(experts * capacity, quarter)[dest]
    picked = picked.astype(jnp.float32).reshape(tok_rows, top, quarter)
    routed = jnp.sum(picked * gate_weights[:, :, None], axis=1)
    return (routed + shared_sum).astype(jnp.bfloat16)


MESH = pl.DeviceIdType.MESH


def silu(v):
    return v / (1.0 + jnp.exp(-v))


def dot32(a, b):
    return jnp.dot(a, b, preferred_element_type=jnp.float32)


def make_kernel(ep_count, capacity, halves):
    others = list(range(1, ep_count))
    part = capacity // halves
    items = list(range(len(others) * halves))

    def kernel(
        tok_ref, gain_ref, routing_ref, gw_ref, wg_hbm, wu_hbm, wd_hbm, sg_hbm, su_hbm, sd_hbm,
        out_ref,
        wg, wu, wd, sg, su, sd, nq, pt, zsend, xq, esend, erecv, keep, fsend, frecv, gsend, grecv,
        wsem, zs, zr, cs, cr, xs, xr, ds, dr, es, er, fs, fr, gs, gr,
    ):
        e = lax.axis_index("ep")
        t = lax.axis_index("tp")
        x = t // 2
        c = t % 2
        core = {"tp": t ^ 1}
        across = {"tp": t ^ 2}
        rows, width = tok_ref.shape
        quarter = width // 4

        def partner(i):
            return {"ep": e ^ (i // halves + 1)}

        barrier = pltpu.get_barrier_semaphore()
        for k in others:
            pl.semaphore_signal(barrier, inc=1, device_id={"ep": e ^ k}, device_id_type=MESH)
        pl.semaphore_signal(barrier, inc=1, device_id=core, device_id_type=MESH)
        pl.semaphore_signal(barrier, inc=1, device_id=across, device_id_type=MESH)

        loads = [
            pltpu.make_async_copy(a, b, wsem.at[i])
            for i, (a, b) in enumerate(
                [(wg_hbm, wg), (wu_hbm, wu), (sg_hbm, sg), (su_hbm, su), (wd_hbm, wd), (sd_hbm, sd)]
            )
        ]
        for load in loads:
            load.start()

        values = tok_ref[...].astype(jnp.float32)
        scale = lax.rsqrt(jnp.mean(values * values, axis=-1, keepdims=True) + 1e-06)
        normed = (values * scale * gain_ref[...]).astype(jnp.bfloat16)
        for q in range(4):
            nq[q] = normed[:, q * quarter:(q + 1) * quarter]

        named = lax.broadcasted_iota(jnp.int32, (16, rows), 0) ^ e
        hit = jnp.zeros((16, rows), jnp.float32)
        weight = jnp.zeros((16, rows), jnp.float32)
        for j in range(routing_ref.shape[0]):
            same = routing_ref[j:j + 1, :] == named
            hit = hit + jnp.where(same, 1.0, 0.0)
            weight = weight + jnp.where(same, gw_ref[j:j + 1, :], 0.0)
        weight = weight.T
        earlier = (
            lax.broadcasted_iota(jnp.int32, (rows, rows), 0)
            < lax.broadcasted_iota(jnp.int32, (rows, rows), 1)
        )
        earlier = jnp.where(earlier, 1.0, 0.0).astype(jnp.bfloat16)
        rank = dot32(hit.astype(jnp.bfloat16), earlier)
        rank = jnp.where(hit > 0.5, rank, -1.0)
        place = lax.broadcasted_iota(jnp.int32, (part, rows), 0)

        def remote(src, dst, send, recv, to):
            return pltpu.make_async_remote_copy(
                src_ref=src, dst_ref=dst, send_sem=send, recv_sem=recv,
                device_id=to, device_id_type=MESH,
            )

        zcopy, ccopy, xcopy, dcopy, ecopy, fcopy, gcopy = {}, {}, {}, {}, {}, {}, {}
        for i in items:
            k, h = i // halves + 1, i % halves
            wanted = (place + h * part).astype(jnp.float32)
            chosen = jnp.where(rank[k:k + 1, :] == wanted, 1.0, 0.0).astype(jnp.bfloat16)
            pt[i] = chosen
            zsend[i] = dot32(chosen, nq[t]).astype(jnp.bfloat16)
            if i == 0:
                pl.semaphore_wait(barrier, len(others) + 2)
            zcopy[i] = remote(zsend.at[i], xq.at[i, t], zs.at[i], zr.at[i], partner(i))
            zcopy[i].start()

        def columns(q):
            return pl.ds(pl.multiple_of(q * quarter, quarter), quarter)

        def hidden_of(pieces, w_gate, w_up):
            gate, up = 0.0, 0.0
            for q in range(4):
                gate = gate + dot32(pieces(q), w_gate[q * quarter:(q + 1) * quarter, :])
                up = up + dot32(pieces(q), w_up[q * quarter:(q + 1) * quarter, :])
            return (silu(gate) * up).astype(jnp.bfloat16)

        def exchange(r, n, product):
            for j in range(2):
                esend[r, j, :n] = product(columns(2 * j + 1 - c)).astype(jnp.bfloat16)
            ecopy[r] = remote(
                esend.at[r, :, pl.ds(0, n)], erecv.at[r, :, pl.ds(0, n)], es.at[r], er.at[r], core
            )
            ecopy[r].start()
            for j in range(2):
                keep[r, j, :n] = product(columns(2 * j + c))

        def arrive(i):
            zcopy[i].wait_recv()
            mine = xq.at[i, t]
            xcopy[i] = remote(mine, mine, xs.at[i], xr.at[i], across)
            xcopy[i].start()
            ccopy[i] = remote(mine, mine, cs.at[i], cr.at[i], core)
            ccopy[i].start()

        def relay(i):
            xcopy[i].wait_recv()
            theirs = xq.at[i, t ^ 2]
            dcopy[i] = remote(theirs, theirs, ds.at[i], dr.at[i], core)
            dcopy[i].start()

        def expert(i):
            ccopy[i].wait_recv()
            dcopy[i].wait_recv()
            hidden = hidden_of(lambda q: xq[i, q], wg, wu)
            exchange(1 + i, part, lambda cols: dot32(hidden, wd[:, cols]))

        def pair(r, n):
            ecopy[r].wait_recv()
            fsend[r, :n] = (
                keep[r, 1 - x, :n] + erecv[r, 1 - x, :n].astype(jnp.float32)
            ).astype(jnp.bfloat16)
            fcopy[r] = remote(
                fsend.at[r, pl.ds(0, n)], frecv.at[r, pl.ds(0, n)], fs.at[r], fr.at[r], across
            )
            fcopy[r].start()

        def whole(r, n):
            fcopy[r].wait_recv()
            return (
                keep[r, x, :n]
                + erecv[r, x, :n].astype(jnp.float32)
                + frecv[r, :n].astype(jnp.float32)
            )

        def give_back(i):
            gsend[i] = whole(1 + i, part).astype(jnp.bfloat16)
            gcopy[i] = remote(gsend.at[i], grecv.at[i], gs.at[i], gr.at[i], partner(i))
            gcopy[i].start()

        for load in loads:
            load.wait()
        own_hidden = hidden_of(lambda q: nq[q], wg, wu)
        shared_hidden = hidden_of(lambda q: nq[q], sg, su)
        exchange(
            0,
            rows,
            lambda cols: dot32(own_hidden, wd[:, cols]) * weight[:, 0:1]
            + dot32(shared_hidden, sd[:, cols]),
        )
        plan(arrive, relay, expert, pair, give_back, len(items), rows, part)

        total = whole(0, rows)
        for i in items:
            k = i // halves + 1
            gcopy[i].wait_recv()
            placed = lax.dot_general(
                pt[i], grecv[i], (((0,), (0,)), ((), ())), preferred_element_type=jnp.float32
            )
            total = total + placed * weight[:, k:k + 1]
        out_ref[...] = total.astype(out_ref.dtype)

        for group in (zcopy, ccopy, xcopy, dcopy, ecopy, fcopy, gcopy):
            for copy in group.values():
                copy.wait_send()

    return kernel


def plan(arrive, relay, expert, pair, give_back, count, rows, part):
    for step in range(count + 3):
        if step < count:
            arrive(step)
        if step == 0:
            pair(0, rows)
        if 0 <= step - 3 < count:
            give_back(step - 3)
        if 0 <= step - 1 < count:
            relay(step - 1)
        if 0 <= step - 2 < count:
            pair(1 + step - 2, part)
        if 0 <= step - 1 < count:
            expert(step - 1)


def fused_body(
    tokens, norm_gain, routing, gate_weights,
    expert_gate, expert_up, expert_down, shared_gate, shared_up, shared_down,
):
    n = lax.axis_size("ep")
    rows, width = tokens.shape
    capacity = max(2, 3 * rows * routing.shape[1] // (2 * n))
    quarter = width // 4
    ffe = expert_gate.shape[2]
    ffs = shared_gate.shape[1]
    halves = 2 if capacity % 32 == 0 else 1
    part = capacity // halves
    o = (n - 1) * halves
    bf16, f32 = jnp.bfloat16, jnp.float32
    big = max(rows, part)
    dma = pltpu.SemaphoreType.DMA
    vmem = pl.BlockSpec(memory_space=pltpu.VMEM)
    hbm = pl.BlockSpec(memory_space=pl.ANY)
    return pl.pallas_call(
        make_kernel(n, capacity, halves),
        out_shape=jax.ShapeDtypeStruct((rows, quarter), bf16),
        in_specs=[vmem] * 4 + [hbm] * 6,
        out_specs=vmem,
        scratch_shapes=[
            pltpu.VMEM((width, ffe), bf16),
            pltpu.VMEM((width, ffe), bf16),
            pltpu.VMEM((ffe, width), bf16),
            pltpu.VMEM((width, ffs), bf16),
            pltpu.VMEM((width, ffs), bf16),
            pltpu.VMEM((ffs, width), bf16),
            pltpu.VMEM((4, rows, quarter), bf16),
            pltpu.VMEM((o, part, rows), bf16),
            pltpu.VMEM((o, part, quarter), bf16),
            pltpu.VMEM((o, 4, part, quarter), bf16),
            pltpu.VMEM((o + 1, 2, big, quarter), bf16),
            pltpu.VMEM((o + 1, 2, big, quarter), bf16),
            pltpu.VMEM((o + 1, 2, big, quarter), f32),
            pltpu.VMEM((o + 1, big, quarter), bf16),
            pltpu.VMEM((o + 1, big, quarter), bf16),
            pltpu.VMEM((o, part, quarter), bf16),
            pltpu.VMEM((o, part, quarter), bf16),
            dma((6,)),
        ]
        + [dma((o,))] * 8
        + [dma((o + 1,))] * 4
        + [dma((o,))] * 2,
        compiler_params=pltpu.CompilerParams(collective_id=0, has_side_effects=True),
    )(
        tokens, norm_gain.reshape(1, width), routing.T, gate_weights.T,
        expert_gate[0], expert_up[0], expert_down[0], shared_gate, shared_up, shared_down,
    )


def solution(mesh):
    in_specs = (
        P(("grp", "ep"), None),
        P(),
        P(("grp", "ep"), None),
        P(("grp", "ep"), None),
        P("ep", None, "tp"),
        P("ep", None, "tp"),
        P("ep", "tp", None),
        P(None, "tp"),
        P(None, "tp"),
        P("tp", None),
    )
    out_specs = P(("grp", "ep"), "tp")
    ep_count, tp_count = mesh.shape["ep"], mesh.shape["tp"]

    def layer(*args):
        few = tp_count == 4 and ep_count in (2, 4) and args[4].shape[0] == ep_count
        chosen = fused_body if few else body
        return jax.shard_map(
            chosen, mesh=mesh, in_specs=in_specs, out_specs=out_specs, check_vma=False
        )(*args)

    return layer
```
